32 devices in a mesh: ep: 8 (over z, x), tp: 4 (over y, core).
Axes of the slice: x: 2, y: 2, z: 4, core: 2. Of those that a mesh axis runs over, the one named last changes fastest.
Arguments:
- queries: bfloat16 [2048, 4096], P('ep', 'tp'), may hold values from -6 to 6
- key_rows: bfloat16 [2048, 4096], P('ep', 'tp'), may hold values from -6 to 6
- value_rows: bfloat16 [2048, 4096], P('ep', 'tp'), may hold values from -6 to 6
- lambdas: float32 [16], P('tp'), may hold values from 0.3 to 0.8
- head_gain: float32 [256], replicated, may hold values from 0.1 to 1.9
- out_proj: bfloat16 [4096, 2048], P('tp'), may hold values from -0.09375 to 0.09375
- moe_input: bfloat16 [1024, 2048], P('ep'), may hold values from -6 to 6
- moe_gain: float32 [2048], replicated, may hold values from 0.1 to 1.9
- routes: int32 [1024, 2], P('ep'), may hold values from 0 to 7, all different within a row; in each aligned block of 32 rows (0 to 31, 32 to 63, ...) at most 16 rows name the same one
- route_weights: float32 [1024, 2], P('ep'), may hold values from 0.2 to 1.2
- expert_gate: bfloat16 [8, 2048, 1024], P('ep', None, 'tp'), may hold values from -0.125 to 0.125
- expert_up: bfloat16 [8, 2048, 1024], P('ep', None, 'tp'), may hold values from -0.125 to 0.125
- expert_down: bfloat16 [8, 1024, 2048], P('ep', 'tp'), may hold values from -0.1875 to 0.1875
- shared_gate: bfloat16 [2048, 1024], P(None, 'tp'), may hold values from -0.125 to 0.125
- shared_up: bfloat16 [2048, 1024], P(None, 'tp'), may hold values from -0.125 to 0.125
- shared_down: bfloat16 [1024, 2048], P('tp'), may hold values from -0.1875 to 0.1875
Outputs:
- mixer_out: bfloat16 [2048, 2048], P(('ep', 'tp'))
- moe_out: bfloat16 [1024, 2048], P(('ep', 'tp'))
The draws below stay inside these ranges and needn't reach their ends.
Inputs may be any that keep to these rules, and one draw needn't show every extreme that they name: `routes`: each row names 2 different experts. The rows of one index of ep fall into 4 aligned blocks of equal size; no expert is named by more than 16 rows of one block, and in every draw some expert is named by exactly 16 rows of some block.
All inputs are finite; a program needn't handle non-finite values.
Results may differ from the reference program's by a relative error of at most 0.02.
Values may be sent and summed in bfloat16 or wider, within the bound.
No kernel may reach another device: no remote copies, remote signals or barrier semaphores. Data moves between devices by JAX's collectives and lax.ppermute only.
A program may use at most 128 MiB of HBM per device.

```python
import math
import jax
import jax.numpy as jnp
import numpy as np
from jax import lax

D = 2048
HEADS = 16
HEAD_DIM = 128
DE = 1024
TOP = 2
TOK2_DEV = 128
TOKENS1 = 2048
TOKENS2 = 1024
EXPERTS = 8
CAP = 16
N_EP = 8
N_TP = 4


def draw_common(key, salt):
    own_key = jax.random.fold_in(key, salt)
    base = jax.random.normal(own_key, (TOKENS1, HEADS * 2 * HEAD_DIM), jnp.float32) * 1.3
    return jnp.clip(base, -6.0, 6.0).astype(jnp.bfloat16)


def draw_queries(key, part):
    return draw_common(key, 11)


def draw_key_rows(key, part):
    return draw_common(key, 12)


def block_levels(rng, shape, pieces, smallest, high):
    def one(axis_at, shards_of):
        steps = jax.random.uniform(jax.random.fold_in(jax.random.fold_in(rng, 6), axis_at), (shards_of,), jnp.float32, smallest / len(pieces), high / len(pieces))
        return jnp.repeat(jnp.exp(steps), shape[axis_at] // shards_of).reshape((-1,) + (1,) * (len(shape) - axis_at - 1))

    level = one(*pieces[0])
    for cut in pieces[1:]:
        level = level * one(*cut)
    return level


def assign_block(rng, own, number, rows, number_of, top, most, skew):
    order = jax.random.permutation(rng, number_of)
    crowded, ordinary = load_shares(number_of, rows * top, most, skew, True), load_shares(number_of, rows * top, most, skew, False)
    places = jnp.arange(number_of)

    def named(sizes, turn):
        used = int((sizes > 0).sum())
        fixed = max(1, used // 4)
        passed = fixed + (places - fixed + turn * (used - fixed)) % max(1, number_of - fixed)
        return jnp.zeros((number_of,), jnp.int32).at[order[jnp.where(places < fixed, places, passed)]].set(jnp.asarray(sizes, jnp.int32))

    sizes = jnp.where(number % 4 == 0, named(crowded, number // 4), named(ordinary, number - number // 4 - 1))
    mixed = jax.random.permutation(jax.random.fold_in(own, 3), number_of)
    giver, receiver = mixed[0:number_of // 2 * 2:2], mixed[1:number_of // 2 * 2:2]
    room = jnp.minimum(sizes[giver] - 1, most - sizes[receiver]) // 2
    room = jnp.where((giver == order[0]) | (receiver == order[0]) | (sizes[receiver] == 0), 0, jnp.maximum(room, 0))
    passed = jax.random.randint(jax.random.fold_in(own, 4), (number_of // 2,), 0, 1 << 20) % (room + 1)
    sizes = sizes.at[giver].add(-passed).at[receiver].add(passed)
    labels = jnp.searchsorted(jnp.cumsum(sizes), jnp.arange(rows * top), side="right").astype(jnp.int32)
    listing = labels.reshape(top, rows).T
    listing = listing[jax.random.permutation(jax.random.fold_in(own, 1), rows)]
    turn = jax.random.randint(jax.random.fold_in(own, 2), (rows, 1), 0, top)
    return jnp.take_along_axis(listing, (jnp.arange(top)[None, :] + turn) % top, axis=1)


def load_shares(amount, total, limit, slope, full):
    weights = [(1 << 20) // math.isqrt(standing ** slope) + 1 for standing in range(1, amount + 1)]
    largest = limit if full else min(limit, max(-(-total // amount), total * weights[0] // sum(weights)))
    least = 1 if total - largest >= amount - 1 else 0
    holding, spare = [largest] + [least] * (amount - 1), total - largest - least * (amount - 1)
    while spare > 0:
        movable = [i for i in range(1, amount) if holding[i] < largest] or [i for i in range(1, amount) if holding[i] < limit]
        mass, budget = sum([weights[i] for i in movable]), spare
        for i in movable:
            addition = min(limit - holding[i], max(1, budget * weights[i] // mass), spare)
            holding[i] = holding[i] + addition
            spare = spare - addition
    return np.array(holding)


def normal_values(key, dims, scale, reach, shards=(), held_as=jnp.bfloat16):
    result = jax.random.normal(key, dims, jnp.float32) * scale
    if len(shards) > 0:
        result = block_levels(key, dims, shards, -0.22, 0.18) * result
    return jnp.clip(result, min=-reach, max=reach).astype(held_as)


def setup_inputs(seed: int = 0) -> dict:
    splits = jax.random.split(jax.random.key(seed), 17)
    queries = draw_queries(jax.random.fold_in(splits[16], 71), 0)
    key_rows = draw_key_rows(jax.random.fold_in(splits[16], 71), 0)
    value_rows = normal_values(splits[2], (TOKENS1, HEADS * 2 * HEAD_DIM), 1.0, 6.0, ((0, 8), (1, 4)))
    lambdas = jnp.clip(0.3 + 0.5 * jax.random.uniform(splits[3], (HEADS,), jnp.float32) ** block_levels(splits[3], (HEADS,), ((0, 4),), -0.2, 0.2), 0.3, 0.8)
    head_gain = jnp.clip(1.0 + 0.18 * jax.random.normal(splits[4], (2 * HEAD_DIM,), jnp.float32), 0.1, 1.9)
    out_proj = normal_values(splits[5], (HEADS * 2 * HEAD_DIM, D), (HEADS * 2 * HEAD_DIM) ** -0.5, 0.09375, ((0, 4),))
    moe_input = normal_values(splits[6], (TOKENS2, D), 1.0, 6.0, ((0, 8),))
    moe_gain = jnp.clip(1.0 + 0.18 * jax.random.normal(splits[7], (D,), jnp.float32), 0.1, 1.9)
    routes_keys = jax.random.split(jax.random.fold_in(splits[8], 1), TOKENS2 // (TOK2_DEV // N_TP))
    routes_turns = jax.random.permutation(jax.random.fold_in(splits[8], 3), TOKENS2 // (TOK2_DEV // N_TP))
    routes = jax.vmap(lambda own, number: assign_block(jax.random.fold_in(splits[8], 2), own, number, TOK2_DEV // N_TP, EXPERTS, TOP, CAP, 2))(routes_keys, routes_turns).reshape((TOKENS2, TOP))
    route_weights = jnp.clip(0.2 + 1 * jax.random.uniform(splits[9], (TOKENS2, TOP), jnp.float32) ** block_levels(splits[9], (TOKENS2, TOP), ((0, 8),), -0.2, 0.2), 0.2, 1.2)
    expert_gate = normal_values(splits[10], (EXPERTS, D, DE), D ** -0.5, 0.125, ((0, 8), (2, 4)))
    expert_up = normal_values(splits[11], (EXPERTS, D, DE), D ** -0.5, 0.125, ((0, 8), (2, 4)))
    expert_down = normal_values(splits[12], (EXPERTS, DE, D), DE ** -0.5, 0.1875, ((0, 8), (1, 4)))
    shared_gate = normal_values(splits[13], (D, DE), D ** -0.5, 0.125, ((1, 4),))
    shared_up = normal_values(splits[14], (D, DE), D ** -0.5, 0.125, ((1, 4),))
    shared_down = normal_values(splits[15], (DE, D), DE ** -0.5, 0.1875, ((0, 4),))
    return dict(queries=queries, key_rows=key_rows, value_rows=value_rows, lambdas=lambdas, head_gain=head_gain, out_proj=out_proj, moe_input=moe_input, moe_gain=moe_gain, routes=routes, route_weights=route_weights, expert_gate=expert_gate, expert_up=expert_up, expert_down=expert_down, shared_gate=shared_gate, shared_up=shared_up, shared_down=shared_down)


theta_base = 500000.0
norm_eps = 1e-06
head_eps = 1e-05

def rotate(matrix, positions, head_dim):
    row_count = matrix.shape[0]
    shaped = matrix.reshape(row_count, -1, head_dim).astype(jnp.float32)
    half_dim = head_dim // 2
    frequency = jnp.power(theta_base, -jnp.arange(half_dim, dtype=jnp.float32) * 2.0 / head_dim)
    angles = positions.astype(jnp.float32)[:, None] * frequency[None, :]
    cosine = jnp.cos(angles)[:, None, :]
    sines = jnp.sin(angles)[:, None, :]
    front_half = shaped[..., :half_dim]
    second = shaped[..., half_dim:]
    turned = jnp.concatenate([front_half * cosine - second * sines, second * cosine + front_half * sines], axis=-1)
    return turned.reshape(matrix.shape).astype(jnp.bfloat16)

def rms_rows(values, gain):
    widened = values.astype(jnp.float32)
    mean_square = lax.optimization_barrier(jnp.mean(widened * widened, axis=-1, keepdims=True))
    return (widened * lax.rsqrt(mean_square + norm_eps) * gain).astype(jnp.bfloat16)

def gated_hidden(rows_in, gate_weight, up_weight):
    gate_part = jnp.dot(rows_in, gate_weight, preferred_element_type=jnp.float32)
    up_part = jnp.dot(rows_in, up_weight, preferred_element_type=jnp.float32)
    return (jax.nn.silu(gate_part) * up_part).astype(jnp.bfloat16)

def grouped_sum(rows_in, weight, groups):
    width = rows_in.shape[1] // groups
    groups_in = jnp.transpose(rows_in.reshape(rows_in.shape[0], groups, width), (1, 0, 2))
    groups_weight = weight.reshape(groups, width, weight.shape[1])

    def add_group(running, operands):
        partial_value = jnp.dot(operands[0], operands[1], preferred_element_type=jnp.float32)
        return (running + lax.optimization_barrier(partial_value.astype(jnp.bfloat16)).astype(jnp.float32), None)
    initial = jnp.zeros((rows_in.shape[0], weight.shape[1]), jnp.float32)
    running, _ = lax.scan(add_group, initial, (groups_in, groups_weight))
    return running

def reference(queries, key_rows, value_rows, lambdas, head_gain, out_proj, moe_input, moe_gain, routes, route_weights, expert_gate, expert_up, expert_down, shared_gate, shared_up, shared_down):
    head_dim = HEAD_DIM
    seq_total = queries.shape[0]
    positions = jnp.arange(seq_total, dtype=jnp.int32)
    rot_query = rotate(queries, positions, head_dim)
    rot_keys = rotate(key_rows, positions, head_dim)
    query_heads = jnp.transpose(rot_query.reshape(seq_total, HEADS, 2, head_dim), (1, 0, 2, 3))
    key_heads = jnp.transpose(rot_keys.reshape(seq_total, HEADS, 2, head_dim), (1, 0, 2, 3))
    value_heads = jnp.transpose(value_rows.reshape(seq_total, HEADS, 2 * head_dim), (1, 0, 2))
    block_rows = 512 if seq_total % 512 == 0 else seq_total

    def one_head(operands):
        head_query, head_keys, head_values, head_lambda = operands
        keys_wide = head_keys.astype(jnp.float32)
        values_wide = head_values.astype(jnp.float32)

        def one_block(block_query):
            scores = jnp.einsum('qmd,kmd->mqk', block_query.astype(jnp.float32), keys_wide) * head_dim ** (-0.5)
            shifted = jnp.exp(scores - lax.optimization_barrier(jnp.max(scores, axis=-1, keepdims=True)))
            denominator = lax.optimization_barrier(jnp.sum(shifted, axis=-1))
            rounded = lax.optimization_barrier(shifted.astype(jnp.bfloat16)).astype(jnp.float32)
            weighted = jnp.einsum('mqk,ke->mqe', rounded, values_wide)
            ratio = weighted / denominator[..., None]
            mixed_heads = ratio[0] - head_lambda * ratio[1]
            mean_square = lax.optimization_barrier(jnp.mean(mixed_heads * mixed_heads, axis=-1, keepdims=True))
            return (mixed_heads * lax.rsqrt(mean_square + head_eps) * head_gain).astype(jnp.bfloat16)
        blocks_out = lax.map(one_block, head_query.reshape(-1, block_rows, 2, head_dim))
        return blocks_out.reshape(seq_total, 2 * head_dim)
    head_out = lax.map(one_head, (query_heads, key_heads, value_heads, lambdas))
    head_out = jnp.transpose(head_out, (1, 0, 2)).reshape(seq_total, HEADS * 2 * head_dim)
    mixer_out = grouped_sum(head_out, out_proj, N_TP).astype(jnp.bfloat16)
    normed = rms_rows(moe_input, moe_gain)
    shared_hidden = gated_hidden(normed, shared_gate, shared_up)
    shared_sum = grouped_sum(shared_hidden, shared_down, N_TP)
    flat_experts = routes.reshape(-1).astype(jnp.int32)
    route_total = flat_experts.shape[0]
    sorted_order = jnp.argsort(flat_experts, stable=True).astype(jnp.int32)
    counts = lax.optimization_barrier(jnp.sum((flat_experts[:, None] == jnp.arange(EXPERTS, dtype=jnp.int32)[None, :]).astype(jnp.int32), axis=0))
    starts = jnp.cumsum(counts) - counts
    sorted_experts = flat_experts[sorted_order]
    slot_place = jnp.zeros((route_total,), jnp.int32).at[sorted_order].set(jnp.arange(route_total, dtype=jnp.int32) - starts[sorted_experts])
    load_bound = N_EP * N_TP * CAP
    table_index = jnp.clip(starts[:, None] + jnp.arange(load_bound, dtype=jnp.int32)[None, :], 0, route_total - 1)
    table_route = sorted_order[table_index]

    def one_expert(operands):
        gate_weight, up_weight, down_weight, route_ids = operands
        rows_in = normed[route_ids // TOP]
        hidden = gated_hidden(rows_in, gate_weight, up_weight)
        return grouped_sum(hidden, down_weight, N_TP).astype(jnp.bfloat16)
    expert_rows = lax.map(one_expert, (expert_gate, expert_up, expert_down, table_route))
    picked = expert_rows[flat_experts, slot_place].reshape(routes.shape[0], TOP, D)
    combined = shared_sum + lax.optimization_barrier(jnp.sum(route_weights[..., None] * picked.astype(jnp.float32), axis=1))
    return (mixer_out, combined.astype(jnp.bfloat16))
```

```python
import jax
import jax.numpy as jnp
from jax import lax
from jax.experimental import pallas as pl
from jax.experimental.pallas import tpu as pltpu
from jax.sharding import PartitionSpec as P

theta_base = 500000.0
norm_eps = 1e-06
head_eps = 1e-05


def rms_rows(values, gain):
    widened = values.astype(jnp.float32)
    mean_square = jnp.mean(widened * widened, axis=-1, keepdims=True)
    return (widened * lax.rsqrt(mean_square + norm_eps) * gain).astype(jnp.bfloat16)


def gated_hidden(rows_in, gate_weight, up_weight):
    gate_part = jnp.dot(rows_in, gate_weight, preferred_element_type=jnp.float32)
    up_part = jnp.dot(rows_in, up_weight, preferred_element_type=jnp.float32)
    return (jax.nn.silu(gate_part) * up_part).astype(jnp.bfloat16)


def swap(pieces, axis):
    count = len(pieces)
    if count <= 8:
        return [pieces[0]] + [
            lax.ppermute(pieces[s], axis, [(j, j ^ s) for j in range(count)])
            for s in range(1, count)
        ]
    order = lax.axis_index(axis) ^ jnp.arange(count, dtype=jnp.int32)
    natural = jnp.take(jnp.stack(pieces), order, axis=0)
    moved = lax.all_to_all(natural, axis, split_axis=0, concat_axis=0, tiled=True)
    return list(jnp.take(moved, order, axis=0))


def rotate_call(queries, key_rows, value_rows, cosine, sines, place, head_count, head_dim):
    rows = queries.shape[0]
    width = 2 * head_dim

    def kernel(place_ref, q_ref, k_ref, v_ref, cos_ref, sin_ref, *outs):
        cosine = cos_ref[...]
        sines = sin_ref[...]
        for s in range(head_count):
            base = pl.multiple_of(((place_ref[0] ^ s) % head_count) * width, width)
            for ref, out in ((k_ref, outs[head_count + s]), (q_ref, outs[s])):
                for m in range(2):
                    part = ref[:, pl.ds(base + m * head_dim, head_dim)].astype(jnp.float32)
                    turned = part * cosine + pltpu.roll(part, head_dim // 2, 1) * sines
                    out[:, m * head_dim : (m + 1) * head_dim] = turned.astype(jnp.bfloat16)
            outs[2 * head_count + s][...] = v_ref[:, pl.ds(base, width)]

    vmem = pl.BlockSpec(memory_space=pltpu.VMEM)
    outs = pl.pallas_call(
        kernel,
        out_shape=[jax.ShapeDtypeStruct((rows, width), jnp.bfloat16)] * (3 * head_count),
        in_specs=[pl.BlockSpec(memory_space=pltpu.SMEM)] + [vmem] * 5,
        out_specs=[vmem] * (3 * head_count),
        cost_estimate=pl.CostEstimate(flops=rows * width * 100, transcendentals=0, bytes_accessed=rows * width * 48),
        name="rotate_split",
    )(place, queries, key_rows, value_rows, cosine, sines)
    return outs[:head_count], outs[head_count : 2 * head_count], outs[2 * head_count :]


def attend_call(q_parts, k_parts, v_parts, lam, head_gain, head_dim):
    rows, width = q_parts[0].shape
    n_q = len(q_parts)
    n_k = len(k_parts)
    factor = head_dim ** (-0.5) * 1.4426950408889634

    def kernel(lam_ref, gain_ref, *refs):
        q_refs = refs[:n_q]
        k_refs = refs[n_q : n_q + n_k]
        v_refs = refs[n_q + n_k : n_q + 2 * n_k]
        o_refs = refs[n_q + 2 * n_k : 2 * n_q + 2 * n_k]
        q_all, o_all = refs[2 * n_q + 2 * n_k :]
        for i in range(n_q):
            q_all[i] = q_refs[i][...]

        def one(i, carry):
            ratios = []
            for m in range(2):
                cols = slice(m * head_dim, (m + 1) * head_dim)
                query = q_all[i, :, cols]
                scores = [
                    lax.dot_general(
                        query, k[:, cols], (((1,), (1,)), ((), ())),
                        preferred_element_type=jnp.float32,
                    )
                    for k in k_refs
                ]
                top = scores[0]
                for part in scores[1:]:
                    top = jnp.maximum(top, part)
                top = jnp.max(top, axis=-1, keepdims=True)
                total = None
                weighted = None
                for part, v in zip(scores, v_refs):
                    weights = jnp.exp2((part - top) * factor)
                    total = weights if total is None else total + weights
                    product = jnp.dot(
                        weights.astype(jnp.bfloat16), v[...], preferred_element_type=jnp.float32
                    )
                    weighted = product if weighted is None else weighted + product
                ratios.append(weighted / jnp.sum(total, axis=-1, keepdims=True))
            mixed = ratios[0] - lam_ref[0] * ratios[1]
            mean_square = jnp.mean(mixed * mixed, axis=-1, keepdims=True)
            o_all[i] = (mixed * lax.rsqrt(mean_square + head_eps) * gain_ref[...]).astype(jnp.bfloat16)
            return carry

        lax.fori_loop(0, n_q, one, 0)
        for i in range(n_q):
            o_refs[i][...] = o_all[i]

    vmem = pl.BlockSpec(memory_space=pltpu.VMEM)
    return pl.pallas_call(
        kernel,
        out_shape=[jax.ShapeDtypeStruct((rows, width), jnp.bfloat16)] * n_q,
        in_specs=[pl.BlockSpec(memory_space=pltpu.SMEM)] + [vmem] * (1 + n_q + 2 * n_k),
        out_specs=[vmem] * n_q,
        scratch_shapes=[pltpu.VMEM((n_q, rows, width), jnp.bfloat16)] * 2,
        cost_estimate=pl.CostEstimate(
            flops=n_q * n_k * rows * rows * width * 6,
            transcendentals=n_q * n_k * rows * rows * 2,
            bytes_accessed=(n_q + n_k) * rows * width * 4,
        ),
        name="attend",
    )(lam, head_gain, *q_parts, *k_parts, *v_parts)


def project_call(parts, weight, places, tp_count):
    rows, width = parts[0].shape
    head_count = len(parts)
    wide = weight.shape[1]
    share = rows // tp_count

    def kernel(places_ref, *refs):
        o_refs = refs[:head_count]
        w_ref = refs[head_count]
        outs = refs[head_count + 1 : head_count + 1 + tp_count]
        scratch = refs[-1]
        total = None
        for s in range(head_count):
            base = pl.multiple_of(((places_ref[0] ^ s) % head_count) * width, width)
            product = jnp.dot(
                o_refs[s][...], w_ref[pl.ds(base, width), :], preferred_element_type=jnp.float32
            )
            total = product if total is None else total + product
        scratch[...] = total.astype(jnp.bfloat16)
        for u in range(tp_count):
            first = pl.multiple_of((places_ref[1] ^ u) * share, share)
            outs[u][...] = scratch[pl.ds(first, share), :]

    vmem = pl.BlockSpec(memory_space=pltpu.VMEM)
    return pl.pallas_call(
        kernel,
        out_shape=[jax.ShapeDtypeStruct((share, wide), jnp.bfloat16)] * tp_count,
        in_specs=[pl.BlockSpec(memory_space=pltpu.SMEM)] + [vmem] * (head_count + 1),
        out_specs=[vmem] * tp_count,
        scratch_shapes=[pltpu.VMEM((rows, wide), jnp.bfloat16)],
        cost_estimate=pl.CostEstimate(
            flops=2 * rows * width * head_count * wide,
            transcendentals=0,
            bytes_accessed=width * head_count * wide * 2 + rows * wide * 2,
        ),
        name="project",
    )(places, *parts, weight)


def slot_table(route_block, experts_order, capacity):
    flat_routes = route_block.reshape(-1)
    route_total = flat_routes.shape[0]
    top_count = route_block.shape[1]
    onehot = (flat_routes[:, None] == experts_order[None, :]).astype(jnp.int32)
    earlier = (
        jnp.arange(route_total)[:, None] > jnp.arange(route_total)[None, :]
    ) & (flat_routes[:, None] == flat_routes[None, :])
    slot_rank = jnp.sum(earlier.astype(jnp.int32), axis=1)
    slot_iota = jnp.arange(capacity, dtype=jnp.int32)
    matches = (onehot.T[:, None, :] > 0) & (slot_rank[None, None, :] == slot_iota[None, :, None])
    pick = jnp.sum(
        matches.reshape(experts_order.shape[0] * capacity, route_total // top_count, top_count),
        axis=2,
    ).astype(jnp.bfloat16)
    return pick, slot_rank.reshape(route_block.shape)


def local(
    queries,
    key_rows,
    value_rows,
    lambdas,
    head_gain,
    out_proj,
    moe_input,
    moe_gain,
    routes,
    route_weights,
    expert_gate,
    expert_up,
    expert_down,
    shared_gate,
    shared_up,
    shared_down,
):
    query_rows = queries.shape[0]
    head_count = lambdas.shape[0]
    head_dim = queries.shape[1] // (2 * head_count)
    tp_count = lax.axis_size("tp")
    ep_count = lax.axis_size("ep")
    tp_place = lax.axis_index("tp")
    ep_place = lax.axis_index("ep")
    places = jnp.stack([ep_place, tp_place]).astype(jnp.int32)

    batch_rows = moe_input.shape[0]
    top_count = routes.shape[1]
    own_rows = batch_rows // tp_count
    local_experts = expert_gate.shape[0]
    expert_count = local_experts * ep_count
    capacity = (2 * own_rows * top_count + expert_count - 1) // expert_count
    own_routes = lax.dynamic_slice_in_dim(routes, tp_place * own_rows, own_rows, 0)
    own_weights = lax.dynamic_slice_in_dim(route_weights, tp_place * own_rows, own_rows, 0)
    experts_order = (
        (ep_place ^ jnp.arange(ep_count, dtype=jnp.int32))[:, None] * local_experts
        + jnp.arange(local_experts, dtype=jnp.int32)[None, :]
    ).reshape(-1)
    pick, own_rank = slot_table(own_routes, experts_order, capacity)
    tp_order = tp_place ^ jnp.arange(tp_count, dtype=jnp.int32)
    ordered = jnp.take(moe_input.reshape(tp_count, own_rows, -1), tp_order, axis=0)
    normed = rms_rows(ordered.reshape(batch_rows, -1), moe_gain)
    outgoing = jnp.dot(pick, normed[:own_rows], preferred_element_type=jnp.float32)
    outgoing = outgoing.astype(jnp.bfloat16).reshape(ep_count, local_experts * capacity, -1)
    arrived = jnp.stack(swap([outgoing[s] for s in range(ep_count)], "ep"))

    positions = (ep_place * query_rows + jnp.arange(query_rows, dtype=jnp.int32)).astype(jnp.float32)
    half_dim = head_dim // 2
    frequency = jnp.power(theta_base, -jnp.arange(half_dim, dtype=jnp.float32) * 2.0 / head_dim)
    angles = positions[:, None] * frequency[None, :]
    cosine = jnp.cos(angles)
    sines = jnp.sin(angles)
    q_parts, k_parts, v_parts = rotate_call(
        queries,
        key_rows,
        value_rows,
        jnp.concatenate([cosine, cosine], axis=1),
        jnp.concatenate([-sines, sines], axis=1),
        places,
        head_count,
        head_dim,
    )
    q_parts = [q_parts[0]] + [
        lax.ppermute(q_parts[s], "ep", [(j, j ^ s) for j in range(ep_count)])
        for s in range(1, head_count)
    ]
    k_parts = swap([k_parts[s % head_count] for s in range(ep_count)], "ep")
    v_parts = swap([v_parts[s % head_count] for s in range(ep_count)], "ep")
    own_lambda = lax.dynamic_slice_in_dim(lambdas, ep_place % head_count, 1, 0)

    shared_hidden = gated_hidden(normed, shared_gate, shared_up)
    shared_part = jnp.dot(shared_hidden, shared_down, preferred_element_type=jnp.float32)
    shared_part = shared_part.astype(jnp.bfloat16).reshape(tp_count, own_rows, -1)
    slot_rows = local_experts * ep_count * capacity
    arrived = arrived.reshape(slot_rows, -1)
    if tp_count == 4:
        cross = lax.ppermute(arrived, "tp", [(j, j ^ 2) for j in range(4)])
        side = lax.ppermute(arrived, "tp", [(j, j ^ 1) for j in range(4)])
        corner = lax.ppermute(cross, "tp", [(j, j ^ 1) for j in range(4)])
        gathered = jnp.stack([arrived, side, cross, corner])
    else:
        gathered = lax.all_gather(arrived, "tp", axis=0, tiled=False)
        gathered = jnp.take(gathered, tp_order, axis=0)
    slots = gathered.reshape(tp_count, ep_count, local_experts, capacity, -1)
    slots = jnp.transpose(slots, (2, 0, 1, 3, 4)).reshape(local_experts, tp_count * ep_count * capacity, -1)
    gate_part = jnp.einsum("xsd,xdf->xsf", slots, expert_gate, preferred_element_type=jnp.float32)
    up_part = jnp.einsum("xsd,xdf->xsf", slots, expert_up, preferred_element_type=jnp.float32)
    hidden = (jax.nn.silu(gate_part) * up_part).astype(jnp.bfloat16)
    routed_part = jnp.einsum("xsf,xfd->xsd", hidden, expert_down, preferred_element_type=jnp.float32)
    routed_part = routed_part.astype(jnp.bfloat16).reshape(
        local_experts, tp_count, ep_count, capacity, -1
    )
    routed_part = jnp.transpose(routed_part, (1, 2, 0, 3, 4)).reshape(tp_count, slot_rows, -1)
    routed_got = swap([routed_part[u] for u in range(tp_count)], "tp")
    shared_got = swap([shared_part[u] for u in range(tp_count)], "tp")
    shared_sum = sum(part.astype(jnp.float32) for part in shared_got)
    routed = sum(part.astype(jnp.float32) for part in routed_got).astype(jnp.bfloat16)
    routed = routed.reshape(ep_count, local_experts * capacity, -1)
    returned = jnp.concatenate(swap([routed[s] for s in range(ep_count)], "ep"), axis=0)

    heads = attend_call(q_parts, k_parts, v_parts, own_lambda, head_gain[None, :], head_dim)
    heads = [heads[0]] + [
        lax.ppermute(heads[s], "ep", [(j, j ^ s) for j in range(ep_count)])
        for s in range(1, head_count)
    ]
    product = project_call(heads, out_proj, places, tp_count)
    mixer_out = sum(part.astype(jnp.float32) for part in swap(list(product), "tp"))
    mixer_out = mixer_out.astype(jnp.bfloat16)

    slot_of = (
        ((own_routes // local_experts) ^ ep_place) * local_experts + own_routes % local_experts
    ) * capacity + own_rank
    place_match = slot_of[:, :, None] == jnp.arange(slot_rows, dtype=jnp.int32)[None, None, :]
    combined = shared_sum
    for k in range(top_count):
        picked = jnp.dot(
            place_match[:, k].astype(jnp.bfloat16), returned, preferred_element_type=jnp.float32
        )
        combined = combined + own_weights[:, k : k + 1] * picked
    return (mixer_out, combined.astype(jnp.bfloat16))


def solution(mesh):
    in_specs = (
        P("ep", "tp"),
        P("ep", "tp"),
        P("ep", "tp"),
        P("tp"),
        P(),
        P("tp", None),
        P("ep", None),
        P(),
        P("ep", None),
        P("ep", None),
        P("ep", None, "tp"),
        P("ep", None, "tp"),
        P("ep", "tp", None),
        P(None, "tp"),
        P(None, "tp"),
        P("tp", None),
    )
    out_specs = (P(("ep", "tp"), None), P(("ep", "tp"), None))
    return jax.shard_map(local, mesh=mesh, in_specs=in_specs, out_specs=out_specs, check_vma=False)
```
